128 devices in a mesh: fs: 16 (over z, y), tp: 8 (over x, core).
Axes of the slice: x: 4, y: 4, z: 4, core: 2. Of those that a mesh axis runs over, the one named last changes fastest.
Arguments:
- saved_input: bfloat16 [262144, 2048], P(('fs', 'tp')), may hold values from -500 to 500
- value_cotangent: bfloat16 [262144, 1024], P(('fs', 'tp')), may hold values from -500 to 500
- hidden_input: bfloat16 [262144, 1024], P(('fs', 'tp')), may hold values from -500 to 500
- out_cotangent: bfloat16 [262144, 2048], P(('fs', 'tp')), may hold values from -500 to 500
- value_factor: bfloat16 [2048, 256], P('fs'), may hold values from -2 to 2
- out_factor: bfloat16 [1024, 256], P('fs'), may hold values from -2 to 2
- value_weight: float32 [2048, 1024], P('fs', 'tp'), may hold values from -0.125 to 0.125
- out_weight: float32 [1024, 2048], P('fs', 'tp'), may hold values from -0.1875 to 0.1875
- value_first: float32 [256, 1024], P('fs', 'tp'), may hold values from -1.2 to 1.2
- value_second: float32 [256, 1024], P('fs', 'tp'), may hold values from 0.02 to 0.5
- out_first: float32 [256, 2048], P('fs', 'tp'), may hold values from -1.2 to 1.2
- out_second: float32 [256, 2048], P('fs', 'tp'), may hold values from 0.02 to 0.5
Outputs:
- value_update: float32 [2048, 1024], P('fs', 'tp')
- out_update: float32 [1024, 2048], P('fs', 'tp')
- new_value_weight: float32 [2048, 1024], P('fs', 'tp')
- new_out_weight: float32 [1024, 2048], P('fs', 'tp')
- value_copy: bfloat16 [2048, 1024], P(None, 'tp')
- out_copy: bfloat16 [1024, 2048], P(None, 'tp')
- new_value_first: float32 [256, 1024], P('fs', 'tp')
- new_value_second: float32 [256, 1024], P('fs', 'tp')
- new_out_first: float32 [256, 2048], P('fs', 'tp')
- new_out_second: float32 [256, 2048], P('fs', 'tp')
The draws below stay inside these ranges and needn't reach their ends.
All inputs are finite; a program needn't handle non-finite values.
Results may differ from the reference program's by a relative error of at most 0.0065.
Values may be sent and summed in bfloat16 or wider, within the bound.
No kernel may reach another device: no remote copies, remote signals or barrier semaphores. Data moves between devices by JAX's collectives and lax.ppermute only.
A program may use at most 128 MiB of HBM per device.

```python
import math
import jax
import jax.numpy as jnp
from jax import lax

D = 2048
DM = 1024
R = 256
TOKENS = 262144


def scaled_field(key, rows, cols, base, row_spread):
    keys = jax.random.split(key, 3)
    field = jnp.clip(jax.random.normal(keys[0], (rows, cols), jnp.float32), -4.0, 4.0)
    row_level = row_spread * jax.random.uniform(keys[1], (rows, 1), jnp.float32)
    column_level = 0.5 * jnp.arange(cols, dtype=jnp.float32)[None, :] / cols
    column_level = column_level + 0.5 * jax.random.uniform(keys[2], (1, cols), jnp.float32)
    return base * field * jnp.power(10.0, row_level + column_level)


def draw_saved_input(key, part):
    return scaled_field(jax.random.fold_in(key, 11), TOKENS, D, 1.0, 1.0).astype(jnp.bfloat16)


def draw_value_cotangent(key, part):
    return scaled_field(jax.random.fold_in(key, 12), TOKENS, DM, 1.0, 1.0).astype(jnp.bfloat16)


def draw_hidden_input(key, part):
    return scaled_field(jax.random.fold_in(key, 13), TOKENS, DM, 1.0, 1.0).astype(jnp.bfloat16)


def draw_out_cotangent(key, part):
    return scaled_field(jax.random.fold_in(key, 14), TOKENS, D, 1.0, 1.0).astype(jnp.bfloat16)


def draw_value_factor(key, part):
    return scaled_field(jax.random.fold_in(key, 15), D, R, 0.04, 0.0).astype(jnp.bfloat16)


def draw_out_factor(key, part):
    return scaled_field(jax.random.fold_in(key, 16), DM, R, 0.04, 0.0).astype(jnp.bfloat16)


def steps_of(key, shape, shards, low, high):
    def one(dim, parts):
        steps = jax.random.uniform(jax.random.fold_in(jax.random.fold_in(key, 6), dim), (parts,), jnp.float32, low / len(shards), high / len(shards))
        return jnp.repeat(jnp.exp(steps), shape[dim] // parts).reshape((-1,) + (1,) * (len(shape) - dim - 1))

    factor_of = one(*shards[0])
    for cut in shards[1:]:
        factor_of = factor_of * one(*cut)
    return factor_of


def centred(key, dims, spread, limit, pieces=(), kind=jnp.bfloat16):
    values = spread * jax.random.normal(key, dims, jnp.float32)
    if pieces:
        values = values * steps_of(key, dims, pieces, -0.22, 0.18)
    return jnp.clip(values, -limit, limit).astype(kind)


def setup_inputs(seed: int = 0) -> dict:
    seeds = jax.random.split(jax.random.key(seed), 13)
    return {
        "saved_input": draw_saved_input(jax.random.fold_in(seeds[12], 71), 0),
        "value_cotangent": draw_value_cotangent(jax.random.fold_in(seeds[12], 71), 0),
        "hidden_input": draw_hidden_input(jax.random.fold_in(seeds[12], 71), 0),
        "out_cotangent": draw_out_cotangent(jax.random.fold_in(seeds[12], 71), 0),
        "value_factor": draw_value_factor(jax.random.fold_in(seeds[12], 71), 0),
        "out_factor": draw_out_factor(jax.random.fold_in(seeds[12], 71), 0),
        "value_weight": centred(seeds[6], (D, DM), D ** -0.5, 0.125, ((0, 16), (1, 8)), jnp.float32),
        "out_weight": centred(seeds[7], (DM, D), DM ** -0.5, 0.1875, ((0, 16), (1, 8)), jnp.float32),
        "value_first": centred(seeds[8], (R, DM), 0.2, 1.2, ((0, 16), (1, 8)), jnp.float32),
        "value_second": jnp.clip(jnp.exp(math.log(0.5) - 3.218876 * jax.random.uniform(seeds[9], (R, DM), jnp.float32) ** steps_of(seeds[9], (R, DM), ((0, 16), (1, 8)), -0.2, 0.2)), 0.02, 0.5),
        "out_first": centred(seeds[10], (R, D), 0.2, 1.2, ((0, 16), (1, 8)), jnp.float32),
        "out_second": jnp.clip(jnp.exp(math.log(0.5) - 3.218876 * jax.random.uniform(seeds[11], (R, D), jnp.float32) ** steps_of(seeds[11], (R, D), ((0, 16), (1, 8)), -0.2, 0.2)), 0.02, 0.5),
    }


momentum_decay = 0.9
square_decay = 0.95
adam_epsilon = 1e-08
update_scale = 0.25
learning_rate = 0.01

def moment_ratio(first, second, lowrank, clip_factor):
    scaled = clip_factor * lowrank
    new_first = momentum_decay * first + (1.0 - momentum_decay) * scaled
    new_second = square_decay * second + (1.0 - square_decay) * scaled * scaled
    ratio = new_first / (jnp.sqrt(new_second) + adam_epsilon)
    return (new_first, new_second, ratio)

def reference(saved_input, value_cotangent, hidden_input, out_cotangent, value_factor, out_factor, value_weight, out_weight, value_first, value_second, out_first, out_second):
    highest = lax.Precision.HIGHEST
    gradient_value = jnp.dot(saved_input.T, value_cotangent, preferred_element_type=jnp.float32)
    gradient_out = jnp.dot(hidden_input.T, out_cotangent, preferred_element_type=jnp.float32)
    value_basis = value_factor.astype(jnp.float32)
    out_basis = out_factor.astype(jnp.float32)
    low_value = jnp.dot(value_basis.T, gradient_value, precision=highest)
    low_out = jnp.dot(out_basis.T, gradient_out, precision=highest)
    total = jnp.sum(low_value * low_value) + jnp.sum(low_out * low_out)
    root_mean = jnp.sqrt(total / (R * (D + DM)))
    clip_factor = 1.0 / jnp.maximum(root_mean, 1.0)
    new_value_first, new_value_second, value_ratio = moment_ratio(value_first, value_second, low_value, clip_factor)
    new_out_first, new_out_second, out_ratio = moment_ratio(out_first, out_second, low_out, clip_factor)
    value_update = update_scale * jnp.dot(value_basis, value_ratio, precision=highest)
    out_update = update_scale * jnp.dot(out_basis, out_ratio, precision=highest)
    new_value_weight = value_weight - learning_rate * value_update
    new_out_weight = out_weight - learning_rate * out_update
    value_copy = new_value_weight.astype(jnp.bfloat16)
    out_copy = new_out_weight.astype(jnp.bfloat16)
    return (value_update, out_update, new_value_weight, new_out_weight, value_copy, out_copy, new_value_first, new_value_second, new_out_first, new_out_second)
```

```python
import jax
import jax.numpy as jnp
from jax import lax
from jax.sharding import Mesh
from jax.sharding import PartitionSpec as P

D = 2048
DM = 1024
R = 256
FS = ("fs_0", "fs_1")
TP = ("tp_0", "tp_1")
CHIPS = ("fs_0", "fs_1", "tp_0")
CORE = "tp_1"
FS_TP = ("fs_0", "fs_1", "tp_0", "tp_1")
HALF = R // 2

momentum_decay = 0.9
square_decay = 0.95
adam_epsilon = 1e-08
update_scale = 0.25
learning_rate = 0.01

bf16 = jnp.bfloat16
f32 = jnp.float32


def exchange(tiles, axis):
    return lax.all_to_all(tiles, axis, split_axis=0, concat_axis=0, tiled=True)


def to_each(block, axis):
    return exchange(jnp.broadcast_to(block, (lax.axis_size(axis), *block.shape)), axis)


def partner(x):
    return lax.ppermute(x, CORE, [(0, 1), (1, 0)])


def side(a):
    return jnp.concatenate([a[:, :128], a[:, 128:]], axis=0)


def unside(a, rows):
    a = a.reshape(16, 2, rows, 128)
    return a.transpose(0, 2, 1, 3).reshape(16 * rows, 256)


def split_dot(factor, ratio):
    high = ratio.astype(bf16)
    rest = (ratio - high.astype(f32)).astype(bf16)
    return jnp.dot(factor, high, preferred_element_type=f32) + jnp.dot(
        factor, rest, preferred_element_type=f32
    )


def moments(first, second, scaled):
    new_first = momentum_decay * first + (1.0 - momentum_decay) * scaled
    new_second = square_decay * second + (1.0 - square_decay) * scaled * scaled
    return new_first, new_second


def columns(a, core):
    width = a.shape[1] // 8
    a = a.reshape(32, 4, 4, 2, width)
    a = jnp.where(core == 0, a, a[:, :, :, ::-1])
    return a.transpose(0, 3, 2, 1, 4)


def shards(
    saved_input,
    value_cotangent,
    hidden_input,
    out_cotangent,
    value_factor,
    out_factor,
    value_weight,
    out_weight,
    value_first,
    value_second,
    out_first,
    out_second,
):
    core = lax.axis_index(CORE)
    row = lax.axis_index(FS)
    factors = jnp.concatenate([value_factor, out_factor], axis=0)
    mine = lax.dynamic_slice(factors, (0, HALF * core), (192, HALF))
    block = jnp.concatenate(
        [
            mine,
            value_weight.astype(bf16),
            side(out_weight.astype(bf16)),
            value_first.astype(bf16),
            value_second.astype(bf16),
            side(out_first.astype(bf16)),
            side(out_second.astype(bf16)),
        ],
        axis=0,
    )
    got = to_each(block, FS)
    factor_mine = got[:, :192]
    factor_other = partner(factor_mine)
    factor = jnp.concatenate([factor_mine, factor_other], axis=2)
    value_f = factor[:, :128].reshape(D, R)
    out_f = factor[:, 128:].reshape(DM, R)
    value_w = got[:, 192:320].reshape(D, 128)
    out_w = unside(got[:, 320:448], 64)
    first_v = got[:, 448:464].reshape(R, 128)
    second_v = got[:, 464:480].reshape(R, 128)
    first_o = unside(got[:, 480:512], 16)
    second_o = unside(got[:, 512:544], 16)

    value_basis = jnp.dot(saved_input, value_f, preferred_element_type=f32).astype(bf16)
    out_basis = jnp.dot(hidden_input, out_f, preferred_element_type=f32).astype(bf16)
    part_v = jnp.einsum("tr,tc->rc", value_basis, value_cotangent, preferred_element_type=f32)
    part_o = jnp.einsum("tr,tc->rc", out_basis, out_cotangent, preferred_element_type=f32)
    sent = jnp.concatenate([part_v[HALF:], part_o[HALF:]], axis=1).astype(bf16)
    came = partner(sent).astype(f32)
    sum_v = (part_v[:HALF] + came[:, :DM]).astype(bf16)
    sum_o = (part_o[:HALF] + came[:, DM:]).astype(bf16)
    tiles = jnp.concatenate([columns(sum_v, core), columns(sum_o, core)], axis=4)
    owned = jnp.sum(exchange(tiles.reshape(64, 16, 384), CHIPS).astype(f32), axis=0)

    squares = jnp.broadcast_to(jnp.sum(owned * owned), (4, 4, 128))
    reply = jnp.concatenate([owned.reshape(4, 12, 128), squares], axis=1)
    replies = jnp.broadcast_to(reply, (16, 4, 16, 128)).reshape(64, 16, 128)
    back = exchange(replies, CHIPS)
    low_mine = back[:, :12].reshape(32, 2, 4, 384)
    ss_mine = jnp.sum(back[:, 12, 0])
    low_kept = low_mine[:, 0].reshape(HALF, 384)
    gone = jnp.concatenate(
        [low_mine[:, 1].reshape(HALF, 384), jnp.broadcast_to(ss_mine, (8, 384))], axis=0
    )
    gone = partner(gone)
    low_other = gone[:HALF]
    total = ss_mine + gone[HALF, 0]
    root_mean = jnp.sqrt(total / (R * (D + DM)))
    clip_factor = 1.0 / jnp.maximum(root_mean, 1.0)
    return low_kept, low_other, clip_factor, value_f, out_f, value_w, out_w, first_v, second_v, first_o, second_o, core, row, (value_weight, out_weight, value_first, value_second, out_first, out_second)


def finish(low_kept, low_other, clip_factor, value_f, out_f, value_w, out_w, first_v, second_v, first_o, second_o, core, row, own):
    value_weight, out_weight, value_first, value_second, out_first, out_second = own
    low = jnp.where(
        core == 0,
        jnp.concatenate([low_kept, low_other], axis=0),
        jnp.concatenate([low_other, low_kept], axis=0),
    )
    scaled = clip_factor * low
    own_scaled = lax.dynamic_slice(scaled, (16 * row, 0), (16, 384))
    new_value_first, new_value_second = moments(value_first, value_second, own_scaled[:, :128])
    new_out_first, new_out_second = moments(out_first, out_second, own_scaled[:, 128:])
    m_v, s_v = moments(first_v.astype(f32), second_v.astype(f32), scaled[:, :128])
    m_o, s_o = moments(first_o.astype(f32), second_o.astype(f32), scaled[:, 128:])
    ratio_v = m_v / (jnp.sqrt(s_v) + adam_epsilon)
    ratio_o = m_o / (jnp.sqrt(s_o) + adam_epsilon)

    def mine_first(a):
        return jnp.where(core == 0, a, jnp.concatenate([a[HALF:], a[:HALF]], axis=0))

    value_all = update_scale * split_dot(value_f, mine_first(ratio_v))
    out_all = update_scale * split_dot(out_f, mine_first(ratio_o))
    value_copy = (value_w.astype(f32) - learning_rate * value_all).astype(bf16)
    out_copy = (out_w.astype(f32) - learning_rate * out_all).astype(bf16)
    value_update = lax.dynamic_slice(value_all, (128 * row, 0), (128, 128))
    out_update = lax.dynamic_slice(out_all, (64 * row, 0), (64, 256))
    return (
        value_update,
        out_update,
        value_weight - learning_rate * value_update,
        out_weight - learning_rate * out_update,
        value_copy,
        out_copy,
        new_value_first,
        new_value_second,
        new_out_first,
        new_out_second,
    )


def step(*args):
    return finish(*shards(*args))


def solution(mesh):
    torus = Mesh(mesh.devices.reshape(4, 4, 4, 2), FS_TP)
    return jax.shard_map(
        step,
        mesh=torus,
        in_specs=(P(FS_TP, None),) * 4 + (P(FS, None),) * 2 + (P(FS, TP),) * 6,
        out_specs=(P(FS, TP),) * 4 + (P(None, TP),) * 2 + (P(FS, TP),) * 4,
        check_vma=False,
    )
```

```python
import jax
import jax.numpy as jnp
from jax import lax
from jax.experimental import pallas as pl
from jax.experimental.pallas import tpu as pltpu
from jax.sharding import Mesh
from jax.sharding import PartitionSpec as P


D = 2048
DM = 1024
R = 256
FS = ("fs_0", "fs_1")
TP = ("tp_0", "tp_1")
CHIPS = ("fs_0", "fs_1", "tp_0")
CORE = "tp_1"
FS_TP = ("fs_0", "fs_1", "tp_0", "tp_1")
HALF = R // 2

momentum_decay = 0.9
square_decay = 0.95
adam_epsilon = 1e-08
update_scale = 0.25
learning_rate = 0.01

bf16 = jnp.bfloat16
f32 = jnp.float32

FACTOR_ROWS = 192
FIRST = (192, 224, 240)
SECOND = (208, 256, 272)
BLOCK_ROWS = 288
VALUE_W = 0
OUT_W = 128
WEIGHT_ROWS = 256


def exchange(tiles, axis):
    return lax.all_to_all(tiles, axis, split_axis=0, concat_axis=0, tiled=True)


def shifted(x, axis):
    out = [x]
    for d in (1, 2, 3):
        out.append(lax.ppermute(x, axis, [(i, (i + d) % 4) for i in range(4)]))
    return out


def near(x):
    return pltpu.with_memory_space_constraint(x, pltpu.VMEM)


def far(x):
    return pltpu.with_memory_space_constraint(x, pltpu.HBM)


def partner(x):
    return lax.ppermute(x, CORE, [(0, 1), (1, 0)])


def call(body, *args, **kwargs):
    def run(*operands):
        return call_of(body, *args, **kwargs)(*operands)

    return run


def call_of(body, out_shape, n_in, scratch=(), smem=1, n_far=0, limit=16, flops=0):
    vmem = pl.BlockSpec(memory_space=pltpu.VMEM)
    many = isinstance(out_shape, (tuple, list))
    return pl.pallas_call(
        body,
        out_shape=out_shape,
        in_specs=[pl.BlockSpec(memory_space=pltpu.SMEM)] * smem
        + [vmem] * n_in
        + [pl.BlockSpec(memory_space=pltpu.HBM)] * n_far,
        out_specs=[vmem] * len(out_shape) if many else vmem,
        scratch_shapes=list(scratch),
        compiler_params=pltpu.CompilerParams(vmem_limit_bytes=limit << 20),
        cost_estimate=pl.CostEstimate(flops=flops, bytes_accessed=0, transcendentals=0)
        if flops
        else None,
    )


def pack_body(at, vf, of, vw, ow, v1, v2, o1, o2, out, weights, block):
    half = pl.ds(pl.multiple_of(HALF * at[0], HALF), HALF)
    block[0:128] = vf[:, half]
    block[128:192] = of[:, half]
    block[192:208] = v1[...].astype(bf16)
    block[208:224] = v2[...].astype(bf16)
    block[224:240] = o1[:, :128].astype(bf16)
    block[240:256] = o1[:, 128:].astype(bf16)
    block[256:272] = o2[:, :128].astype(bf16)
    block[272:288] = o2[:, 128:].astype(bf16)
    for k in range(16):
        out[k] = block[...]
    weights[0:128] = vw[...].astype(bf16)
    weights[128:192] = ow[:, :128].astype(bf16)
    weights[192:256] = ow[:, 128:].astype(bf16)


def place_body(at, w0, w1, w2, w3, out):
    row = at[1]
    for dz, part in enumerate((w0, w1, w2, w3)):
        for dy in range(4):
            from_z = jnp.bitwise_and(row // 4 - dz, 3)
            from_y = jnp.bitwise_and(row - dy, 3)
            out[4 * from_z + from_y] = part[dy]


def join_factors(mine, other, fv, fo):
    for lanes, part in ((slice(0, 128), mine), (slice(128, 256), other)):
        for k in range(16):
            fv[128 * k : 128 * k + 128, lanes] = part[k, 0:128]
            fo[64 * k : 64 * k + 64, lanes] = part[k, 128:192]


def arrange(acc, first_row, core, out):
    low_rows = lax.broadcasted_iota(jnp.int32, (16, 8, 128), 1) < 4
    for h in range(2):
        column = jnp.bitwise_xor(core, h)
        for j in range(3):
            quads = []
            for x in range(4):
                if j == 0:
                    start = 256 * x + 128 * column
                else:
                    start = DM + 512 * x + 256 * column + 128 * (j - 1)
                lanes = pl.ds(pl.multiple_of(start, 128), 128)
                quads.append(acc[first_row : first_row + HALF, lanes].reshape(16, 8, 128))
            rolled = [pltpu.roll(q, 4, 1) for q in quads]
            low = [
                jnp.where(low_rows, quads[0], rolled[1]),
                jnp.where(low_rows, quads[2], rolled[3]),
            ]
            high = [
                jnp.where(low_rows, rolled[0], quads[1]),
                jnp.where(low_rows, rolled[2], quads[3]),
            ]
            lanes = slice(128 * j, 128 * j + 128)
            out[:, 2 * h, :, lanes] = jnp.concatenate(low, axis=1).astype(out.dtype)
            out[:, 2 * h + 1, :, lanes] = jnp.concatenate(high, axis=1).astype(out.dtype)


ACROSS = (((0,), (0,)), ((), ()))


def tokens_body(
    at, mine, other, x_far, c_far, h_far, o_far,
    kept, sent, fv, fo, acc, vb, ob, x, c, h, o, sems,
):
    step = x.shape[0] // 4

    def rows(i):
        return pl.ds(pl.multiple_of(i * step, step), step)

    def lanes(i):
        return pl.ds(pl.multiple_of(i * 512, 512), 512)

    def h_copy(i):
        return pltpu.make_async_copy(h_far.at[rows(i)], h.at[rows(i)], sems.at[i])

    def c_copy(i):
        return pltpu.make_async_copy(c_far.at[:, lanes(i)], c.at[:, lanes(i)], sems.at[4 + i])

    def o_copy(i):
        return pltpu.make_async_copy(o_far.at[:, lanes(i)], o.at[:, lanes(i)], sems.at[6 + i])

    def x_copy(i):
        return pltpu.make_async_copy(x_far.at[rows(i)], x.at[rows(i)], sems.at[10 + i])

    for i in range(4):
        h_copy(i).start()
    x_copy(0).start()
    join_factors(mine, other, fv, fo)

    def saved(i, carry):
        x_copy(i).wait()
        o_copy(i).start()
        vb[rows(i)] = jnp.dot(x[rows(i)], fv[...], preferred_element_type=f32).astype(bf16)
        return carry

    def hidden(i, carry):
        h_copy(i).wait()

        @pl.when(i < 3)
        def _():
            x_copy(i + 1).start()

        ob[rows(i)] = jnp.dot(h[rows(i)], fo[...], preferred_element_type=f32).astype(bf16)
        return carry

    def value_part(i, carry):
        c_copy(i).wait()
        acc[:, lanes(i)] = lax.dot_general(
            vb[...], c[:, lanes(i)], ACROSS, preferred_element_type=f32
        )
        return carry

    def out_part(i, carry):
        o_copy(i).wait()
        acc[:, pl.ds(pl.multiple_of(DM + i * 512, 512), 512)] = lax.dot_general(
            ob[...], o[:, lanes(i)], ACROSS, preferred_element_type=f32
        )
        return carry

    lax.fori_loop(0, 4, hidden, 0)
    c_copy(0).start()
    c_copy(1).start()
    lax.fori_loop(0, 4, saved, 0)
    lax.fori_loop(0, 2, value_part, 0)
    lax.fori_loop(0, 4, out_part, 0)
    arrange(acc, HALF, 1 - at[0], sent)
    arrange(acc, 0, at[0], kept)


def reply_body(tiles, out, own, stage):
    own[...] = jnp.sum(tiles[...].astype(f32), axis=0)
    squares = jnp.sum(own[...] * own[...])
    for x in range(4):
        for j in range(3):
            stage[x, 4 * j : 4 * j + 4] = own[4 * x : 4 * x + 4, 128 * j : 128 * j + 128]
        stage[x, 12:16] = jnp.full((4, 128), squares, f32)
    for k in range(16):
        out[4 * k : 4 * k + 4] = stage[...]


def sum_of_squares(back):
    return jnp.sum(back[:, :, 12:16]) * (1.0 / 512.0)


def hand_body(back, out):
    out[...] = back[:, 2:4]
    out[:, :, 12:16] = jnp.full((16, 2, 4, 128), sum_of_squares(back), f32)


def moments(first, second, scaled):
    new_first = momentum_decay * first + (1.0 - momentum_decay) * scaled
    new_second = square_decay * second + (1.0 - square_decay) * scaled * scaled
    return new_first, new_second


def finish_body(
    at, back, came, got, other, weights, vw, ow, v1, v2, o1, o2,
    vup, oup, nvw, now, vcopy, ocopy, nv1, nv2, no1, no2,
    low, fv, fo, ratios, vall, oall,
):
    core, row, start = at[0], at[1], at[2]
    total = sum_of_squares(back) + came[0, 0, 12, 0]
    root_mean = jnp.sqrt(jnp.full((8, 128), total, f32) / (R * (D + DM)))
    clip_factor = (1.0 / jnp.maximum(root_mean, 1.0))[0:1]

    low_rows = lax.broadcasted_iota(jnp.int32, (16, 8, 128), 1) < 4
    for half, part in ((0, back), (1, came)):
        shard = pl.ds(8 * jnp.bitwise_xor(core, half), 8)
        ranks = slice(HALF * half, HALF * half + HALF)
        a, b = part[:, 0], part[:, 1]
        joined = (
            jnp.where(low_rows, a[:, :8], pltpu.roll(b[:, :8], 4, 1)),
            jnp.where(low_rows, pltpu.roll(a[:, :8], 4, 1), b[:, :8]),
            jnp.where(low_rows, a[:, 8:], pltpu.roll(b[:, 8:], 4, 1)),
        )
        for j in range(3):
            scaled = joined[j].reshape(HALF, 128) * clip_factor
            low[ranks, 128 * j : 128 * j + 128] = scaled
            first = got[shard, FIRST[j] : FIRST[j] + 16].astype(f32).reshape(HALF, 128)
            second = got[shard, SECOND[j] : SECOND[j] + 16].astype(f32).reshape(HALF, 128)
            first, second = moments(first, second, scaled)
            ratio = first / (jnp.sqrt(second) + adam_epsilon)
            high = ratio.astype(bf16)
            rest = (ratio - high.astype(f32)).astype(bf16)
            at_high, at_rest = ((0, 128), (256, 512), (384, 640))[j]
            ratios[ranks, at_high : at_high + 128] = high
            ratios[ranks, at_rest : at_rest + 128] = rest

    own = pl.ds(pl.multiple_of(start, 16), 16)
    nv1[...], nv2[...] = moments(v1[...], v2[...], low[own, 0:128])
    no1[...], no2[...] = moments(o1[...], o2[...], low[own, 128:384])

    join_factors(got, other, fv, fo)
    for k in range(4):
        rows = slice(512 * k, 512 * k + 512)
        both = jnp.dot(fv[rows], ratios[:, 0:256], preferred_element_type=f32)
        update = update_scale * (both[:, :128] + both[:, 128:])
        vall[rows] = update
        weight = weights[4 * k : 4 * k + 4, VALUE_W : VALUE_W + 128].astype(f32).reshape(512, 128)
        vcopy[rows] = (weight - learning_rate * update).astype(bf16)
    for k in range(2):
        rows = slice(512 * k, 512 * k + 512)
        both = jnp.dot(fo[rows], ratios[:, 256:768], preferred_element_type=f32)
        update = update_scale * (both[:, :256] + both[:, 256:])
        oall[rows] = update
        for side in range(2):
            lanes = slice(128 * side, 128 * side + 128)
            at_w = OUT_W + 64 * side
            weight = weights[8 * k : 8 * k + 8, at_w : at_w + 64].astype(f32).reshape(512, 128)
            ocopy[rows, lanes] = (weight - learning_rate * update[:, lanes]).astype(bf16)

    update = vall[pl.ds(pl.multiple_of(128 * row, 128), 128)]
    vup[...] = update
    nvw[...] = vw[...] - learning_rate * update
    update = oall[pl.ds(pl.multiple_of(64 * row, 64), 64)]
    oup[...] = update
    now[...] = ow[...] - learning_rate * update


def shards(x, c, h, o, vf, of, vw, ow, v1, v2, o1, o2):
    core = lax.axis_index(CORE)
    row = lax.axis_index(FS)
    start = HALF * jnp.bitwise_xor(row // 8, core) + 16 * (row % 8)
    at = jnp.stack([core, row, start]).astype(jnp.int32)

    blocks, weights = call(
        pack_body,
        (pltpu.VMEM((16, BLOCK_ROWS, 128), bf16), pltpu.VMEM((WEIGHT_ROWS, 128), bf16)),
        8,
        [pltpu.VMEM((BLOCK_ROWS, 128), bf16)],
    )(at, *map(far, (vf, of, vw, ow, v1, v2, o1, o2)))
    got = exchange(blocks, FS)
    got, weights = lax.optimization_barrier((got, weights))
    other = partner(got[:, :FACTOR_ROWS])
    along_y = jnp.stack(shifted(weights, "fs_1"))
    parts = shifted(along_y, "fs_0")

    kept, sent = call(
        tokens_body,
        (pltpu.VMEM((16, 4, 16, 384), f32), pltpu.VMEM((16, 4, 16, 384), bf16)),
        2,
        [
            pltpu.VMEM((D, R), bf16),
            pltpu.VMEM((DM, R), bf16),
            pltpu.VMEM((R, D + DM), f32),
            pltpu.VMEM((x.shape[0], R), bf16),
            pltpu.VMEM((x.shape[0], R), bf16),
            pltpu.VMEM(x.shape, bf16),
            pltpu.VMEM(c.shape, bf16),
            pltpu.VMEM(h.shape, bf16),
            pltpu.VMEM(o.shape, bf16),
            pltpu.SemaphoreType.DMA((14,)),
        ],
        n_far=4,
        limit=36,
        flops=12 * x.shape[0] * D * R,
    )(at, near(got), near(other), far(x), far(c), far(h), far(o))
    came = partner(sent)
    tiles = (kept + came.astype(f32)).astype(bf16)
    tiles = exchange(tiles.reshape(64, 16, 384), CHIPS)
    replies = call(
        reply_body,
        pltpu.VMEM((64, 16, 128), f32),
        1,
        [pltpu.VMEM((16, 384), f32), pltpu.VMEM((4, 16, 128), f32)],
        smem=0,
    )(near(tiles))
    back = exchange(replies, CHIPS).reshape(16, 4, 16, 128)
    back = near(back)
    weights = call(place_body, pltpu.VMEM((16, WEIGHT_ROWS, 128), bf16), 4)(
        at, *[near(p) for p in parts]
    )
    came = partner(call(hand_body, pltpu.VMEM((16, 2, 16, 128), f32), 1, smem=0)(back))

    def like(a, dtype=f32):
        return jax.ShapeDtypeStruct(a.shape, dtype)

    return call(
        finish_body,
        (
            like(vw),
            like(ow),
            like(vw),
            like(ow),
            jax.ShapeDtypeStruct((D, 128), bf16),
            jax.ShapeDtypeStruct((DM, 256), bf16),
            like(v1),
            like(v2),
            like(o1),
            like(o2),
        ),
        11,
        [
            pltpu.VMEM((R, 384), f32),
            pltpu.VMEM((D, R), bf16),
            pltpu.VMEM((DM, R), bf16),
            pltpu.VMEM((R, 768), bf16),
            pltpu.VMEM((D, 128), f32),
            pltpu.VMEM((DM, 256), f32),
        ],
    )(at, back, near(came), near(got), near(other), near(weights), vw, ow, v1, v2, o1, o2)


def solution(mesh):
    torus = Mesh(mesh.devices.reshape(4, 4, 4, 2), FS_TP)
    return jax.shard_map(
        shards,
        mesh=torus,
        in_specs=(P(FS_TP, None),) * 4 + (P(FS, None),) * 2 + (P(FS, TP),) * 6,
        out_specs=(P(FS, TP),) * 4 + (P(None, TP),) * 2 + (P(FS, TP),) * 4,
        check_vma=False,
    )
```

```python
import jax
import jax.numpy as jnp
from jax import lax
from jax.experimental import pallas as pl
from jax.experimental.pallas import tpu as pltpu
from jax.sharding import Mesh
from jax.sharding import PartitionSpec as P


D = 2048
DM = 1024
R = 256
FS = ("fs_0", "fs_1")
TP = ("tp_0", "tp_1")
CHIPS = ("fs_0", "fs_1", "tp_0")
CORE = "tp_1"
FS_TP = ("fs_0", "fs_1", "tp_0", "tp_1")
HALF = R // 2

momentum_decay = 0.9
square_decay = 0.95
adam_epsilon = 1e-08
update_scale = 0.25
learning_rate = 0.01

bf16 = jnp.bfloat16
f32 = jnp.float32

BLOCK_ROWS = 192
VALUE_W = 0
OUT_W = 128
FIRST = (256, 288, 304)
SECOND = (272, 320, 336)
STATE_ROWS = 352


def exchange(tiles, axis):
    return lax.all_to_all(tiles, axis, split_axis=0, concat_axis=0, tiled=True)


def shift(x, axis, d):
    return lax.ppermute(x, axis, [(i, (i + d) % 4) for i in range(4)])


def near(x):
    return pltpu.with_memory_space_constraint(x, pltpu.VMEM)


def far(x):
    return pltpu.with_memory_space_constraint(x, pltpu.HBM)


def partner(x):
    return lax.ppermute(x, CORE, [(0, 1), (1, 0)])


def call(body, *args, **kwargs):
    def run(*operands):
        return call_of(body, *args, **kwargs)(*operands)

    return run


def call_of(body, out_shape, n_in, scratch=(), smem=1, n_far=0, limit=16, flops=0):
    vmem = pl.BlockSpec(memory_space=pltpu.VMEM)
    many = isinstance(out_shape, (tuple, list))
    return pl.pallas_call(
        body,
        out_shape=out_shape,
        in_specs=[pl.BlockSpec(memory_space=pltpu.SMEM)] * smem
        + [vmem] * n_in
        + [pl.BlockSpec(memory_space=pltpu.HBM)] * n_far,
        out_specs=[vmem] * len(out_shape) if many else vmem,
        scratch_shapes=list(scratch),
        compiler_params=pltpu.CompilerParams(vmem_limit_bytes=limit << 20),
        cost_estimate=pl.CostEstimate(flops=flops, bytes_accessed=0, transcendentals=0)
        if flops
        else None,
    )


def pack_body(at, vf, of, vw, ow, v1, v2, o1, o2, out, state, block):
    half = pl.ds(pl.multiple_of(HALF * at[0], HALF), HALF)
    block[0:128] = vf[:, half]
    block[128:192] = of[:, half]
    for k in range(16):
        out[k] = block[...]
    state[0:128] = vw[...].astype(bf16)
    state[128:192] = ow[:, :128].astype(bf16)
    state[192:256] = ow[:, 128:].astype(bf16)
    state[256:272] = v1[...].astype(bf16)
    state[272:288] = v2[...].astype(bf16)
    state[288:304] = o1[:, :128].astype(bf16)
    state[304:320] = o1[:, 128:].astype(bf16)
    state[320:336] = o2[:, :128].astype(bf16)
    state[336:352] = o2[:, 128:].astype(bf16)


def place_body(at, w0, w1, up, down, w3, out):
    row = at[1]
    for dz in range(4):
        for dy in range(4):
            from_z = jnp.bitwise_and(row // 4 - dz, 3)
            from_y = jnp.bitwise_and(row - dy, 3)
            if dz == 2:
                part = up[dy] if dy < 2 else down[dy - 2]
            else:
                part = (w0, w1, None, w3)[dz][dy]
            out[4 * from_z + from_y] = part


def join_factors(mine, other, fv, fo):
    for lanes, part in ((slice(0, 128), mine), (slice(128, 256), other)):
        for k in range(16):
            fv[128 * k : 128 * k + 128, lanes] = part[k, 0:128]
            fo[64 * k : 64 * k + 64, lanes] = part[k, 128:192]


def arrange(acc, first_row, core, out):
    low_rows = lax.broadcasted_iota(jnp.int32, (16, 8, 128), 1) < 4
    for h in range(2):
        column = jnp.bitwise_xor(core, h)
        for j in range(3):
            quads = []
            for x in range(4):
                if j == 0:
                    start = 256 * x + 128 * column
                else:
                    start = DM + 512 * x + 256 * column + 128 * (j - 1)
                lanes = pl.ds(pl.multiple_of(start, 128), 128)
                quads.append(acc[first_row : first_row + HALF, lanes].reshape(16, 8, 128))
            rolled = [pltpu.roll(q, 4, 1) for q in quads]
            low = [
                jnp.where(low_rows, quads[0], rolled[1]),
                jnp.where(low_rows, quads[2], rolled[3]),
            ]
            high = [
                jnp.where(low_rows, rolled[0], quads[1]),
                jnp.where(low_rows, rolled[2], quads[3]),
            ]
            lanes = slice(128 * j, 128 * j + 128)
            out[:, 2 * h, :, lanes] = jnp.concatenate(low, axis=1).astype(out.dtype)
            out[:, 2 * h + 1, :, lanes] = jnp.concatenate(high, axis=1).astype(out.dtype)


ACROSS = (((0,), (0,)), ((), ()))


def tokens_body(
    at, mine, other, x_far, c_far, h_far, o_far,
    kept, sent, fv, fo, acc, vb, ob, x, c, h, o, sems,
):
    step = x.shape[0] // 4

    def rows(i):
        return pl.ds(pl.multiple_of(i * step, step), step)

    def lanes(i):
        return pl.ds(pl.multiple_of(i * 512, 512), 512)

    def h_copy(i):
        return pltpu.make_async_copy(h_far.at[rows(i)], h.at[rows(i)], sems.at[i])

    def c_copy(i):
        return pltpu.make_async_copy(c_far.at[:, lanes(i)], c.at[:, lanes(i)], sems.at[4 + i])

    def o_copy(i):
        return pltpu.make_async_copy(o_far.at[:, lanes(i)], o.at[:, lanes(i)], sems.at[6 + i])

    def x_copy(i):
        return pltpu.make_async_copy(x_far.at[rows(i)], x.at[rows(i)], sems.at[10 + i])

    for i in range(4):
        h_copy(i).start()
    x_copy(0).start()
    join_factors(mine, other, fv, fo)

    def saved(i, carry):
        x_copy(i).wait()
        o_copy(i).start()
        vb[rows(i)] = jnp.dot(x[rows(i)], fv[...], preferred_element_type=f32).astype(bf16)
        return carry

    def hidden(i, carry):
        h_copy(i).wait()

        @pl.when(i < 3)
        def _():
            x_copy(i + 1).start()

        ob[rows(i)] = jnp.dot(h[rows(i)], fo[...], preferred_element_type=f32).astype(bf16)
        return carry

    def value_part(carry):
        c_copy(0).wait()
        c_copy(1).wait()
        acc[:, :DM] = lax.dot_general(vb[...], c[...], ACROSS, preferred_element_type=f32)
        return carry

    def out_part(i, carry):
        o_copy(2 * i).wait()
        o_copy(2 * i + 1).wait()
        at_in = pl.ds(pl.multiple_of(i * 1024, 1024), 1024)
        at_out = pl.ds(pl.multiple_of(DM + i * 1024, 1024), 1024)
        acc[:, at_out] = lax.dot_general(
            ob[...], o[:, at_in], ACROSS, preferred_element_type=f32
        )
        return carry

    lax.fori_loop(0, 4, hidden, 0)
    c_copy(0).start()
    c_copy(1).start()
    lax.fori_loop(0, 4, saved, 0)
    value_part(0)
    lax.fori_loop(0, 2, out_part, 0)
    arrange(acc, HALF, 1 - at[0], sent)
    arrange(acc, 0, at[0], kept)


def halves_body(replies, before, after, up, down):
    up[...] = before[0:2]
    down[...] = after[2:4]


def reply_body(tiles, out, own, stage):
    own[...] = jnp.sum(tiles[...].astype(f32), axis=0)
    squares = jnp.sum(own[...] * own[...])
    for x in range(4):
        for j in range(3):
            stage[x, 4 * j : 4 * j + 4] = own[4 * x : 4 * x + 4, 128 * j : 128 * j + 128]
        stage[x, 12:16] = jnp.full((4, 128), squares, f32)
    for k in range(16):
        out[4 * k : 4 * k + 4] = stage[...]


def sum_of_squares(back):
    return jnp.sum(back[:, :, 12:16]) * (1.0 / 512.0)


def hand_body(back, out):
    out[...] = back[:, 2:4]
    out[:, :, 12:16] = jnp.full((16, 2, 4, 128), sum_of_squares(back), f32)


def moments(first, second, scaled):
    new_first = momentum_decay * first + (1.0 - momentum_decay) * scaled
    new_second = square_decay * second + (1.0 - square_decay) * scaled * scaled
    return new_first, new_second


def finish_body(
    at, back, came, fv, fo, weights, vw, ow, v1, v2, o1, o2,
    vup, oup, nvw, now, vcopy, ocopy, nv1, nv2, no1, no2,
    low, ratios, vall, oall,
):
    core, row, start = at[0], at[1], at[2]
    total = sum_of_squares(back) + came[0, 0, 12, 0]
    root_mean = jnp.sqrt(jnp.full((8, 128), total, f32) / (R * (D + DM)))
    clip_factor = (1.0 / jnp.maximum(root_mean, 1.0))[0:1]

    low_rows = lax.broadcasted_iota(jnp.int32, (16, 8, 128), 1) < 4
    for half, part in ((0, back), (1, came)):
        shard = pl.ds(8 * jnp.bitwise_xor(core, half), 8)
        ranks = slice(HALF * half, HALF * half + HALF)
        a, b = part[:, 0], part[:, 1]
        joined = (
            jnp.where(low_rows, a[:, :8], pltpu.roll(b[:, :8], 4, 1)),
            jnp.where(low_rows, pltpu.roll(a[:, :8], 4, 1), b[:, :8]),
            jnp.where(low_rows, a[:, 8:], pltpu.roll(b[:, 8:], 4, 1)),
        )
        for j in range(3):
            scaled = joined[j].reshape(HALF, 128) * clip_factor
            low[ranks, 128 * j : 128 * j + 128] = scaled
            first = weights[shard, FIRST[j] : FIRST[j] + 16].astype(f32).reshape(HALF, 128)
            second = weights[shard, SECOND[j] : SECOND[j] + 16].astype(f32).reshape(HALF, 128)
            first, second = moments(first, second, scaled)
            ratio = first / (jnp.sqrt(second) + adam_epsilon)
            high = ratio.astype(bf16)
            rest = (ratio - high.astype(f32)).astype(bf16)
            at_high, at_rest = ((0, 128), (256, 512), (384, 640))[j]
            ratios[ranks, at_high : at_high + 128] = high
            ratios[ranks, at_rest : at_rest + 128] = rest

    own = pl.ds(pl.multiple_of(start, 16), 16)
    nv1[...], nv2[...] = moments(v1[...], v2[...], low[own, 0:128])
    no1[...], no2[...] = moments(o1[...], o2[...], low[own, 128:384])

    for k in range(4):
        rows = slice(512 * k, 512 * k + 512)
        both = jnp.dot(fv[rows], ratios[:, 0:256], preferred_element_type=f32)
        update = update_scale * (both[:, :128] + both[:, 128:])
        vall[rows] = update
        weight = weights[4 * k : 4 * k + 4, VALUE_W : VALUE_W + 128].astype(f32).reshape(512, 128)
        vcopy[rows] = (weight - learning_rate * update).astype(bf16)
    for k in range(2):
        rows = slice(512 * k, 512 * k + 512)
        both = jnp.dot(fo[rows], ratios[:, 256:768], preferred_element_type=f32)
        update = update_scale * (both[:, :256] + both[:, 256:])
        oall[rows] = update
        for side in range(2):
            lanes = slice(128 * side, 128 * side + 128)
            at_w = OUT_W + 64 * side
            weight = weights[8 * k : 8 * k + 8, at_w : at_w + 64].astype(f32).reshape(512, 128)
            ocopy[rows, lanes] = (weight - learning_rate * update[:, lanes]).astype(bf16)

    update = vall[pl.ds(pl.multiple_of(128 * row, 128), 128)]
    vup[...] = update
    nvw[...] = vw[...] - learning_rate * update
    update = oall[pl.ds(pl.multiple_of(64 * row, 64), 64)]
    oup[...] = update
    now[...] = ow[...] - learning_rate * update


def shards(x, c, h, o, vf, of, vw, ow, v1, v2, o1, o2):
    core = lax.axis_index(CORE)
    row = lax.axis_index(FS)
    start = HALF * jnp.bitwise_xor(row // 8, core) + 16 * (row % 8)
    at = jnp.stack([core, row, start]).astype(jnp.int32)

    blocks, weights = call(
        pack_body,
        (pltpu.VMEM((16, BLOCK_ROWS, 128), bf16), pltpu.VMEM((STATE_ROWS, 128), bf16)),
        8,
        [pltpu.VMEM((BLOCK_ROWS, 128), bf16)],
    )(at, *map(far, (vf, of, vw, ow, v1, v2, o1, o2)))
    got = exchange(blocks, FS)
    got, weights = lax.optimization_barrier((got, weights))
    other = partner(got)
    along_y = jnp.stack([weights] + [shift(weights, "fs_1", d) for d in (1, 2, 3)])
    before = shift(along_y, "fs_0", 1)
    after = shift(along_y, "fs_0", 3)

    kept, sent, fv, fo = call(
        tokens_body,
        (
            pltpu.VMEM((16, 4, 16, 384), f32),
            pltpu.VMEM((16, 4, 16, 384), bf16),
            pltpu.VMEM((D, R), bf16),
            pltpu.VMEM((DM, R), bf16),
        ),
        2,
        [
            pltpu.VMEM((R, D + DM), f32),
            pltpu.VMEM((x.shape[0], R), bf16),
            pltpu.VMEM((x.shape[0], R), bf16),
            pltpu.VMEM(x.shape, bf16),
            pltpu.VMEM(c.shape, bf16),
            pltpu.VMEM(h.shape, bf16),
            pltpu.VMEM(o.shape, bf16),
            pltpu.SemaphoreType.DMA((14,)),
        ],
        n_far=4,
        limit=36,
        flops=12 * x.shape[0] * D * R,
    )(at, near(got), near(other), far(x), far(c), far(h), far(o))
    came = partner(sent)
    tiles = (kept + came.astype(f32)).astype(bf16)
    tiles = exchange(tiles.reshape(64, 16, 384), CHIPS)
    pair = pltpu.VMEM((2, STATE_ROWS, 128), bf16)
    replies = call(
        reply_body,
        pltpu.VMEM((64, 16, 128), f32),
        1,
        [pltpu.VMEM((16, 384), f32), pltpu.VMEM((4, 16, 128), f32)],
        smem=0,
    )(near(tiles))
    up, down = call(halves_body, (pair, pair), 3, smem=0)(near(replies), near(before), near(after))
    up = shift(up, "fs_0", 1)
    down = shift(down, "fs_0", 3)
    back = exchange(replies, CHIPS).reshape(16, 4, 16, 128)
    back = near(back)
    weights = call(place_body, pltpu.VMEM((16, STATE_ROWS, 128), bf16), 5)(
        at, *map(near, (along_y, before, up, down, after))
    )
    came = partner(call(hand_body, pltpu.VMEM((16, 2, 16, 128), f32), 1, smem=0)(back))

    def like(a, dtype=f32):
        return jax.ShapeDtypeStruct(a.shape, dtype)

    return call(
        finish_body,
        (
            like(vw),
            like(ow),
            like(vw),
            like(ow),
            jax.ShapeDtypeStruct((D, 128), bf16),
            jax.ShapeDtypeStruct((DM, 256), bf16),
            like(v1),
            like(v2),
            like(o1),
            like(o2),
        ),
        11,
        [
            pltpu.VMEM((R, 384), f32),
            pltpu.VMEM((R, 768), bf16),
            pltpu.VMEM((D, 128), f32),
            pltpu.VMEM((DM, 256), f32),
        ],
    )(at, back, near(came), near(fv), near(fo), near(weights), vw, ow, v1, v2, o1, o2)


def solution(mesh):
    torus = Mesh(mesh.devices.reshape(4, 4, 4, 2), FS_TP)
    return jax.shard_map(
        shards,
        mesh=torus,
        in_specs=(P(FS_TP, None),) * 4 + (P(FS, None),) * 2 + (P(FS, TP),) * 6,
        out_specs=(P(FS, TP),) * 4 + (P(None, TP),) * 2 + (P(FS, TP),) * 4,
        check_vma=False,
    )
```

```python
import jax
import jax.numpy as jnp
from jax import lax
from jax.experimental import pallas as pl
from jax.experimental.pallas import tpu as pltpu
from jax.sharding import Mesh
from jax.sharding import PartitionSpec as P


D = 2048
DM = 1024
R = 256
FS = ("fs_0", "fs_1")
TP = ("tp_0", "tp_1")
CHIPS = ("fs_0", "fs_1", "tp_0")
CORE = "tp_1"
FS_TP = ("fs_0", "fs_1", "tp_0", "tp_1")
HALF = R // 2

momentum_decay = 0.9
square_decay = 0.95
adam_epsilon = 1e-08
update_scale = 0.25
learning_rate = 0.01

bf16 = jnp.bfloat16
f32 = jnp.float32

BLOCK_ROWS = 192
VALUE_W = 0
OUT_W = 128
FIRST = (256, 288, 304)
SECOND = (272, 320, 336)
STATE_ROWS = 352


def exchange(tiles, axis):
    return lax.all_to_all(tiles, axis, split_axis=0, concat_axis=0, tiled=True)


def shift(x, axis, d):
    return lax.ppermute(x, axis, [(i, (i + d) % 4) for i in range(4)])


def near(x):
    return pltpu.with_memory_space_constraint(x, pltpu.VMEM)


def far(x):
    return pltpu.with_memory_space_constraint(x, pltpu.HBM)


def partner(x):
    return lax.ppermute(x, CORE, [(0, 1), (1, 0)])


def call(body, *args, **kwargs):
    def run(*operands):
        return call_of(body, *args, **kwargs)(*operands)

    return run


def call_of(body, out_shape, n_in, scratch=(), smem=1, n_far=0, limit=16, flops=0):
    vmem = pl.BlockSpec(memory_space=pltpu.VMEM)
    many = isinstance(out_shape, (tuple, list))
    return pl.pallas_call(
        body,
        out_shape=out_shape,
        in_specs=[pl.BlockSpec(memory_space=pltpu.SMEM)] * smem
        + [vmem] * n_in
        + [pl.BlockSpec(memory_space=pltpu.HBM)] * n_far,
        out_specs=[vmem] * len(out_shape) if many else vmem,
        scratch_shapes=list(scratch),
        compiler_params=pltpu.CompilerParams(vmem_limit_bytes=limit << 20),
        cost_estimate=pl.CostEstimate(flops=flops, bytes_accessed=0, transcendentals=0)
        if flops
        else None,
    )


def pack_body(at, vf, of, vw, ow, v1, v2, o1, o2, out, state, block):
    half = pl.ds(pl.multiple_of(HALF * at[0], HALF), HALF)
    block[0:128] = vf[:, half]
    block[128:192] = of[:, half]
    for k in range(16):
        out[k] = block[...]
    state[0:128] = vw[...].astype(bf16)
    state[128:192] = ow[:, :128].astype(bf16)
    state[192:256] = ow[:, 128:].astype(bf16)
    state[256:272] = v1[...].astype(bf16)
    state[272:288] = v2[...].astype(bf16)
    state[288:304] = o1[:, :128].astype(bf16)
    state[304:320] = o1[:, 128:].astype(bf16)
    state[320:336] = o2[:, :128].astype(bf16)
    state[336:352] = o2[:, 128:].astype(bf16)


def place_body(at, w0, w1, w2, w3, out):
    row = at[1]
    for dz in range(4):
        for dy in range(4):
            from_z = jnp.bitwise_and(row // 4 - dz, 3)
            from_y = jnp.bitwise_and(row - dy, 3)
            out[4 * from_z + from_y] = (w0, w1, w2, w3)[dz][dy]


def join_factors(mine, other, fv, fo):
    for lanes, part in ((slice(0, 128), mine), (slice(128, 256), other)):
        for k in range(16):
            fv[128 * k : 128 * k + 128, lanes] = part[k, 0:128]
            fo[64 * k : 64 * k + 64, lanes] = part[k, 128:192]


def arrange(acc, first_row, core, out):
    low_rows = lax.broadcasted_iota(jnp.int32, (16, 8, 128), 1) < 4
    for h in range(2):
        column = jnp.bitwise_xor(core, h)
        for j in range(3):
            quads = []
            for x in range(4):
                if j == 0:
                    start = 256 * x + 128 * column
                else:
                    start = DM + 512 * x + 256 * column + 128 * (j - 1)
                lanes = pl.ds(pl.multiple_of(start, 128), 128)
                quads.append(acc[first_row : first_row + HALF, lanes].reshape(16, 8, 128))
            rolled = [pltpu.roll(q, 4, 1) for q in quads]
            low = [
                jnp.where(low_rows, quads[0], rolled[1]),
                jnp.where(low_rows, quads[2], rolled[3]),
            ]
            high = [
                jnp.where(low_rows, rolled[0], quads[1]),
                jnp.where(low_rows, rolled[2], quads[3]),
            ]
            lanes = slice(128 * j, 128 * j + 128)
            out[:, 2 * h, :, lanes] = jnp.concatenate(low, axis=1).astype(out.dtype)
            out[:, 2 * h + 1, :, lanes] = jnp.concatenate(high, axis=1).astype(out.dtype)


ACROSS = (((0,), (0,)), ((), ()))


def tokens_body(
    at, mine, other, x_far, c_far, h_far, o_far,
    kept, sent, fv, fo, acc, vb, ob, x, c, h, o, sems,
):
    step = x.shape[0] // 4

    def rows(i):
        return pl.ds(pl.multiple_of(i * step, step), step)

    def lanes(i):
        return pl.ds(pl.multiple_of(i * 512, 512), 512)

    def h_copy(i):
        return pltpu.make_async_copy(h_far.at[rows(i)], h.at[rows(i)], sems.at[i])

    def c_copy(i):
        return pltpu.make_async_copy(c_far.at[:, lanes(i)], c.at[:, lanes(i)], sems.at[4 + i])

    def o_copy(i):
        return pltpu.make_async_copy(o_far.at[:, lanes(i)], o.at[:, lanes(i)], sems.at[6 + i])

    def x_copy(i):
        return pltpu.make_async_copy(x_far.at[rows(i)], x.at[rows(i)], sems.at[10 + i])

    for i in range(4):
        h_copy(i).start()
    x_copy(0).start()
    join_factors(mine, other, fv, fo)

    def saved(i, carry):
        x_copy(i).wait()
        o_copy(i).start()
        vb[rows(i)] = jnp.dot(x[rows(i)], fv[...], preferred_element_type=f32).astype(bf16)
        return carry

    def hidden(i, carry):
        h_copy(i).wait()

        @pl.when(i < 3)
        def _():
            x_copy(i + 1).start()

        ob[rows(i)] = jnp.dot(h[rows(i)], fo[...], preferred_element_type=f32).astype(bf16)
        return carry

    def value_part(carry):
        c_copy(0).wait()
        c_copy(1).wait()
        acc[:, :DM] = lax.dot_general(vb[...], c[...], ACROSS, preferred_element_type=f32)
        return carry

    def out_part(i, carry):
        o_copy(2 * i).wait()
        o_copy(2 * i + 1).wait()
        at_in = pl.ds(pl.multiple_of(i * 1024, 1024), 1024)
        at_out = pl.ds(pl.multiple_of(DM + i * 1024, 1024), 1024)
        acc[:, at_out] = lax.dot_general(
            ob[...], o[:, at_in], ACROSS, preferred_element_type=f32
        )
        return carry

    lax.fori_loop(0, 4, hidden, 0)
    c_copy(0).start()
    c_copy(1).start()
    lax.fori_loop(0, 4, saved, 0)
    value_part(0)
    lax.fori_loop(0, 2, out_part, 0)
    arrange(acc, HALF, 1 - at[0], sent)
    arrange(acc, 0, at[0], kept)


def onward_body(replies, before, up):
    up[...] = before[...]


def reply_body(tiles, out, own, stage):
    own[...] = jnp.sum(tiles[...].astype(f32), axis=0)
    squares = jnp.sum(own[...] * own[...])
    for x in range(4):
        for j in range(3):
            stage[x, 4 * j : 4 * j + 4] = own[4 * x : 4 * x + 4, 128 * j : 128 * j + 128]
        stage[x, 12:16] = jnp.full((4, 128), squares, f32)
    for k in range(16):
        out[4 * k : 4 * k + 4] = stage[...]


def sum_of_squares(back):
    return jnp.sum(back[:, :, 12:16]) * (1.0 / 512.0)


def hand_body(back, out):
    out[...] = back[:, 2:4]
    out[:, :, 12:16] = jnp.full((16, 2, 4, 128), sum_of_squares(back), f32)


def moments(first, second, scaled):
    new_first = momentum_decay * first + (1.0 - momentum_decay) * scaled
    new_second = square_decay * second + (1.0 - square_decay) * scaled * scaled
    return new_first, new_second


def finish_body(
    at, back, came, fv, fo, weights, vw, ow, v1, v2, o1, o2,
    vup, oup, nvw, now, vcopy, ocopy, nv1, nv2, no1, no2,
    low, ratios, vall, oall,
):
    core, row, start = at[0], at[1], at[2]
    total = sum_of_squares(back) + came[0, 0, 12, 0]
    root_mean = jnp.sqrt(jnp.full((8, 128), total, f32) / (R * (D + DM)))
    clip_factor = (1.0 / jnp.maximum(root_mean, 1.0))[0:1]

    low_rows = lax.broadcasted_iota(jnp.int32, (16, 8, 128), 1) < 4
    for half, part in ((0, back), (1, came)):
        shard = pl.ds(8 * jnp.bitwise_xor(core, half), 8)
        ranks = slice(HALF * half, HALF * half + HALF)
        a, b = part[:, 0], part[:, 1]
        joined = (
            jnp.where(low_rows, a[:, :8], pltpu.roll(b[:, :8], 4, 1)),
            jnp.where(low_rows, pltpu.roll(a[:, :8], 4, 1), b[:, :8]),
            jnp.where(low_rows, a[:, 8:], pltpu.roll(b[:, 8:], 4, 1)),
        )
        for j in range(3):
            scaled = joined[j].reshape(HALF, 128) * clip_factor
            low[ranks, 128 * j : 128 * j + 128] = scaled
            first = weights[shard, FIRST[j] : FIRST[j] + 16].astype(f32).reshape(HALF, 128)
            second = weights[shard, SECOND[j] : SECOND[j] + 16].astype(f32).reshape(HALF, 128)
            first, second = moments(first, second, scaled)
            ratio = first / (jnp.sqrt(second) + adam_epsilon)
            high = ratio.astype(bf16)
            rest = (ratio - high.astype(f32)).astype(bf16)
            at_high, at_rest = ((0, 128), (256, 512), (384, 640))[j]
            ratios[ranks, at_high : at_high + 128] = high
            ratios[ranks, at_rest : at_rest + 128] = rest

    own = pl.ds(pl.multiple_of(start, 16), 16)
    nv1[...], nv2[...] = moments(v1[...], v2[...], low[own, 0:128])
    no1[...], no2[...] = moments(o1[...], o2[...], low[own, 128:384])

    for k in range(4):
        rows = slice(512 * k, 512 * k + 512)
        both = jnp.dot(fv[rows], ratios[:, 0:256], preferred_element_type=f32)
        update = update_scale * (both[:, :128] + both[:, 128:])
        vall[rows] = update
        weight = weights[4 * k : 4 * k + 4, VALUE_W : VALUE_W + 128].astype(f32).reshape(512, 128)
        vcopy[rows] = (weight - learning_rate * update).astype(bf16)
    for k in range(2):
        rows = slice(512 * k, 512 * k + 512)
        both = jnp.dot(fo[rows], ratios[:, 256:768], preferred_element_type=f32)
        update = update_scale * (both[:, :256] + both[:, 256:])
        oall[rows] = update
        for side in range(2):
            lanes = slice(128 * side, 128 * side + 128)
            at_w = OUT_W + 64 * side
            weight = weights[8 * k : 8 * k + 8, at_w : at_w + 64].astype(f32).reshape(512, 128)
            ocopy[rows, lanes] = (weight - learning_rate * update[:, lanes]).astype(bf16)

    update = vall[pl.ds(pl.multiple_of(128 * row, 128), 128)]
    vup[...] = update
    nvw[...] = vw[...] - learning_rate * update
    update = oall[pl.ds(pl.multiple_of(64 * row, 64), 64)]
    oup[...] = update
    now[...] = ow[...] - learning_rate * update


def shards(x, c, h, o, vf, of, vw, ow, v1, v2, o1, o2):
    core = lax.axis_index(CORE)
    row = lax.axis_index(FS)
    start = HALF * jnp.bitwise_xor(row // 8, core) + 16 * (row % 8)
    at = jnp.stack([core, row, start]).astype(jnp.int32)

    blocks, weights = call(
        pack_body,
        (pltpu.VMEM((16, BLOCK_ROWS, 128), bf16), pltpu.VMEM((STATE_ROWS, 128), bf16)),
        8,
        [pltpu.VMEM((BLOCK_ROWS, 128), bf16)],
    )(at, *map(far, (vf, of, vw, ow, v1, v2, o1, o2)))
    got = exchange(blocks, FS)
    got, weights = lax.optimization_barrier((got, weights))
    other = partner(got)
    along_y = jnp.stack([weights] + [shift(weights, "fs_1", d) for d in (1, 2, 3)])
    before = shift(along_y, "fs_0", 1)
    after = shift(along_y, "fs_0", 3)

    kept, sent, fv, fo = call(
        tokens_body,
        (
            pltpu.VMEM((16, 4, 16, 384), f32),
            pltpu.VMEM((16, 4, 16, 384), bf16),
            pltpu.VMEM((D, R), bf16),
            pltpu.VMEM((DM, R), bf16),
        ),
        2,
        [
            pltpu.VMEM((R, D + DM), f32),
            pltpu.VMEM((x.shape[0], R), bf16),
            pltpu.VMEM((x.shape[0], R), bf16),
            pltpu.VMEM(x.shape, bf16),
            pltpu.VMEM(c.shape, bf16),
            pltpu.VMEM(h.shape, bf16),
            pltpu.VMEM(o.shape, bf16),
            pltpu.SemaphoreType.DMA((14,)),
        ],
        n_far=4,
        limit=36,
        flops=12 * x.shape[0] * D * R,
    )(at, near(got), near(other), far(x), far(c), far(h), far(o))
    came = partner(sent)
    tiles = (kept + came.astype(f32)).astype(bf16)
    tiles = exchange(tiles.reshape(64, 16, 384), CHIPS)
    replies = call(
        reply_body,
        pltpu.VMEM((64, 16, 128), f32),
        1,
        [pltpu.VMEM((16, 384), f32), pltpu.VMEM((4, 16, 128), f32)],
        smem=0,
    )(near(tiles))
    line = pltpu.VMEM((4, STATE_ROWS, 128), bf16)
    onward = call(onward_body, line, 2, smem=0)(near(replies), near(before))
    onward = shift(onward, "fs_0", 1)
    back = exchange(replies, CHIPS).reshape(16, 4, 16, 128)
    back = near(back)
    weights = call(place_body, pltpu.VMEM((16, STATE_ROWS, 128), bf16), 4)(
        at, *map(near, (along_y, before, onward, after))
    )
    came = partner(call(hand_body, pltpu.VMEM((16, 2, 16, 128), f32), 1, smem=0)(back))

    def like(a, dtype=f32):
        return jax.ShapeDtypeStruct(a.shape, dtype)

    return call(
        finish_body,
        (
            like(vw),
            like(ow),
            like(vw),
            like(ow),
            jax.ShapeDtypeStruct((D, 128), bf16),
            jax.ShapeDtypeStruct((DM, 256), bf16),
            like(v1),
            like(v2),
            like(o1),
            like(o2),
        ),
        11,
        [
            pltpu.VMEM((R, 384), f32),
            pltpu.VMEM((R, 768), bf16),
            pltpu.VMEM((D, 128), f32),
            pltpu.VMEM((DM, 256), f32),
        ],
    )(at, back, near(came), near(fv), near(fo), near(weights), vw, ow, v1, v2, o1, o2)


def solution(mesh):
    torus = Mesh(mesh.devices.reshape(4, 4, 4, 2), FS_TP)
    return jax.shard_map(
        shards,
        mesh=torus,
        in_specs=(P(FS_TP, None),) * 4 + (P(FS, None),) * 2 + (P(FS, TP),) * 6,
        out_specs=(P(FS, TP),) * 4 + (P(None, TP),) * 2 + (P(FS, TP),) * 4,
        check_vma=False,
    )
```
